32 devices in a mesh: sp: 8 (over z, x), tp: 4 (over y, core).
Axes of the slice: x: 2, y: 2, z: 4, core: 2. Of those that a mesh axis runs over, the one named last changes fastest.
Arguments:
- query_maps: bfloat16 [1536, 1024], P('sp', 'tp'), may hold values from -6 to 6
- key_maps: bfloat16 [1536, 512], P('sp', 'tp'), may hold values from -6 to 6
- value_rows: bfloat16 [1536, 512], P('sp', 'tp'), may hold values from -6 to 6
- mix_lambda: float32 [8], P('tp'), may hold values from 0.3 to 0.8
- head_gain: float32 [128], replicated, may hold values from 0.1 to 1.9
- out_weight: bfloat16 [1024, 2048], replicated, may hold values from -0.1875 to 0.1875
- residual: bfloat16 [1536, 2048], P(('sp', 'tp')), may hold values from -6 to 6
- norm_gain: float32 [2048], replicated, may hold values from 0.1 to 1.9
- routes: int32 [1536, 4], P('sp'), may hold values from 0 to 7, all different within a row; in each aligned block of 48 rows (0 to 47, 48 to 95, ...) at most 48 rows name the same one
- route_weight: float32 [1536, 4], P(('sp', 'tp')), may hold values from 0.3 to 1.5
- expert_gate: bfloat16 [8, 2048, 1024], P('sp', None, 'tp'), may hold values from -0.125 to 0.125
- expert_up: bfloat16 [8, 2048, 1024], P('sp', None, 'tp'), may hold values from -0.125 to 0.125
- expert_down: bfloat16 [8, 1024, 2048], P('sp', 'tp'), may hold values from -0.1875 to 0.1875
- shared_gate: bfloat16 [2048, 1024], P(None, 'tp'), may hold values from -0.125 to 0.125
- shared_up: bfloat16 [2048, 1024], P(None, 'tp'), may hold values from -0.125 to 0.125
- shared_down: bfloat16 [1024, 2048], P('tp'), may hold values from -0.1875 to 0.1875
Outputs:
- mixed: bfloat16 [1536, 2048], P(('sp', 'tp'))
The draws below stay inside these ranges and needn't reach their ends.
Inputs may be any that keep to these rules, and one draw needn't show every extreme that they name: `routes`: the 4 experts of a token are different. In each aligned block of 48 tokens (the tokens of one device after the attention) no expert is named more than 48 times, a bound that some expert reaches in some blocks.
All inputs are finite; a program needn't handle non-finite values.
Results may differ from the reference program's by a relative error of at most 0.018.
Values may be sent and summed in bfloat16 or wider, within the bound.
A program may use at most 128 MiB of HBM per device.

```python
import math
import jax
import jax.numpy as jnp
import numpy as np
from jax import lax

D = 2048
HEADS = 8
KV_HEADS = 4
HD = 64
VD = 128
EXPERTS = 8
EXP_FF = 1024
SH_FF = 1024
TOP_K = 4
SEQ = 1536
ROWS_DEV = 48
CAP = 48
N_TP = 4


def base_values(key, salt, shape):
    values = jnp.clip(1.3 * jax.random.normal(jax.random.fold_in(key, salt), shape, jnp.float32), -6.0, 6.0)
    return values


def draw_key_maps(key, part):
    values = base_values(key, 7010, (SEQ, KV_HEADS * 2 * HD))
    return values.astype(jnp.bfloat16)


def draw_query_maps(key, part):
    values = base_values(key, 7020, (SEQ, HEADS * 2 * HD))
    return values.astype(jnp.bfloat16)


def levels(own_key, extent, pieces, low, top_value):
    def one(dim, shards_of):
        heights = jax.random.uniform(jax.random.fold_in(jax.random.fold_in(own_key, 6), dim), (shards_of,), jnp.float32, low / len(pieces), top_value / len(pieces))
        return jnp.repeat(jnp.exp(heights), extent[dim] // shards_of).reshape((-1,) + (1,) * (len(extent) - dim - 1))

    factor_of = one(*pieces[0])
    for cut in pieces[1:]:
        factor_of = factor_of * one(*cut)
    return factor_of


def routed_block(own_key, own, number, rows, amount, top, bound, skew):
    sequence = jax.random.permutation(own_key, amount)
    packed, ordinary = shares(amount, rows * top, bound, skew, True), shares(amount, rows * top, bound, skew, False)
    places = jnp.arange(amount)

    def named(sizes, offset_by):
        used = int((sizes > 0).sum())
        fixed = max(1, used // 4)
        shifted = fixed + (places - fixed + offset_by * (used - fixed)) % max(1, amount - fixed)
        return jnp.zeros((amount,), jnp.int32).at[sequence[jnp.where(places < fixed, places, shifted)]].set(jnp.asarray(sizes, jnp.int32))

    sizes = jnp.where(number % 4 == 0, named(packed, number // 4), named(ordinary, number - number // 4 - 1))
    mixed = jax.random.permutation(jax.random.fold_in(own, 3), amount)
    giver, taker = mixed[0:amount // 2 * 2:2], mixed[1:amount // 2 * 2:2]
    room = jnp.minimum(sizes[giver] - 1, bound - sizes[taker]) // 2
    room = jnp.where((giver == sequence[0]) | (taker == sequence[0]) | (sizes[taker] == 0), 0, jnp.maximum(room, 0))
    shifted = jax.random.randint(jax.random.fold_in(own, 4), (amount // 2,), 0, 1 << 20) % (room + 1)
    sizes = sizes.at[giver].add(-shifted).at[taker].add(shifted)
    members = jnp.searchsorted(jnp.cumsum(sizes), jnp.arange(rows * top), side="right").astype(jnp.int32)
    grid = members.reshape(top, rows).T
    grid = grid[jax.random.permutation(jax.random.fold_in(own, 1), rows)]
    offset_by = jax.random.randint(jax.random.fold_in(own, 2), (rows, 1), 0, top)
    return jnp.take_along_axis(grid, (jnp.arange(top)[None, :] + offset_by) % top, axis=1)


def shares(count, total, most, lean, full):
    portions = [(1 << 20) // math.isqrt(standing ** lean) + 1 for standing in range(1, count + 1)]
    largest = most if full else min(most, max(-(-total // count), total * portions[0] // sum(portions)))
    least = 1 if total - largest >= count - 1 else 0
    holding, surplus = [largest] + [least] * (count - 1), total - largest - least * (count - 1)
    while surplus > 0:
        candidates = [i for i in range(1, count) if holding[i] < largest] or [i for i in range(1, count) if holding[i] < most]
        mass, left = sum([portions[i] for i in candidates]), surplus
        for i in candidates:
            more = min(most - holding[i], max(1, left * portions[i] // mass), surplus)
            holding[i] = holding[i] + more
            surplus = surplus - more
    return np.array(holding)


def bell_draw(key, dims, spread, reach, shards=(), held_as=jnp.bfloat16):
    result = jax.random.normal(key, dims, jnp.float32) * spread
    if len(shards) > 0:
        result = levels(key, dims, shards, -0.22, 0.18) * result
    return jnp.clip(result, min=-reach, max=reach).astype(held_as)


def setup_inputs(seed: int = 0) -> dict:
    arg_keys = jax.random.split(jax.random.key(seed), 17)
    query_maps = draw_query_maps(jax.random.fold_in(arg_keys[16], 71), 0)
    key_maps = draw_key_maps(jax.random.fold_in(arg_keys[16], 71), 0)
    value_rows = bell_draw(arg_keys[2], (SEQ, KV_HEADS * VD), 1.0, 6.0, ((0, 8), (1, 4)))
    mix_lambda = jnp.clip(0.3 + 0.5 * jax.random.uniform(arg_keys[3], (HEADS,), jnp.float32) ** levels(arg_keys[3], (HEADS,), ((0, 4),), -0.2, 0.2), 0.3, 0.8)
    head_gain = jnp.clip(1.0 + 0.18 * jax.random.normal(arg_keys[4], (VD,), jnp.float32), 0.1, 1.9)
    out_weight = bell_draw(arg_keys[5], (HEADS * VD, D), (HEADS * VD) ** -0.5, 0.1875)
    residual = bell_draw(arg_keys[6], (SEQ, D), 1.0, 6.0, ((0, 32),))
    norm_gain = jnp.clip(1.0 + 0.18 * jax.random.normal(arg_keys[7], (D,), jnp.float32), 0.1, 1.9)
    routes_keys = jax.random.split(jax.random.fold_in(arg_keys[8], 1), SEQ // ROWS_DEV)
    routes_turns = jax.random.permutation(jax.random.fold_in(arg_keys[8], 3), SEQ // ROWS_DEV)
    routes = jax.vmap(lambda own, number: routed_block(jax.random.fold_in(arg_keys[8], 2), own, number, ROWS_DEV, EXPERTS, TOP_K, CAP, 2))(routes_keys, routes_turns).reshape((SEQ, TOP_K))
    route_weight = jnp.clip(jnp.exp(math.log(1.5) - 1.60943787 * jax.random.uniform(arg_keys[9], (SEQ, TOP_K), jnp.float32) ** levels(arg_keys[9], (SEQ, TOP_K), ((0, 32),), -0.2, 0.2)), 0.3, 1.5)
    expert_gate = bell_draw(arg_keys[10], (EXPERTS, D, EXP_FF), D ** -0.5, 0.125, ((0, 8), (2, 4)))
    expert_up = bell_draw(arg_keys[11], (EXPERTS, D, EXP_FF), D ** -0.5, 0.125, ((0, 8), (2, 4)))
    expert_down = bell_draw(arg_keys[12], (EXPERTS, EXP_FF, D), EXP_FF ** -0.5, 0.1875, ((0, 8), (1, 4)))
    shared_gate = bell_draw(arg_keys[13], (D, SH_FF), D ** -0.5, 0.125, ((1, 4),))
    shared_up = bell_draw(arg_keys[14], (D, SH_FF), D ** -0.5, 0.125, ((1, 4),))
    shared_down = bell_draw(arg_keys[15], (SH_FF, D), SH_FF ** -0.5, 0.1875, ((0, 4),))
    return dict(query_maps=query_maps, key_maps=key_maps, value_rows=value_rows, mix_lambda=mix_lambda, head_gain=head_gain, out_weight=out_weight, residual=residual, norm_gain=norm_gain, routes=routes, route_weight=route_weight, expert_gate=expert_gate, expert_up=expert_up, expert_down=expert_down, shared_gate=shared_gate, shared_up=shared_up, shared_down=shared_down)


norm_eps = 1e-06

def slot_targets(block_routes):
    flat_routes = block_routes.reshape(-1)
    onehot = (flat_routes[:, None] == jnp.arange(EXPERTS, dtype=jnp.int32)[None, :]).astype(jnp.int32)
    earlier = jnp.cumsum(onehot, axis=0) - onehot
    return (flat_routes, lax.optimization_barrier(jnp.sum(earlier * onehot, axis=1)).astype(jnp.int32))

def grouped_feedforward(token_rows, gate_weight, up_weight, down_weight):
    gate_value = jnp.dot(token_rows, gate_weight, preferred_element_type=jnp.float32)
    up_value = jnp.dot(token_rows, up_weight, preferred_element_type=jnp.float32)
    hidden = (jax.nn.silu(gate_value) * up_value).astype(jnp.bfloat16)
    group_width = hidden.shape[1] // N_TP
    running = jnp.zeros((token_rows.shape[0], down_weight.shape[1]), jnp.float32)
    for group_index in range(N_TP):
        partial_sum = jnp.dot(hidden[:, group_index * group_width:(group_index + 1) * group_width], down_weight[group_index * group_width:(group_index + 1) * group_width], preferred_element_type=jnp.float32)
        running = running + lax.optimization_barrier(partial_sum.astype(jnp.bfloat16)).astype(jnp.float32)
    return running.astype(jnp.bfloat16)

def head_attention(query_maps, key_maps, value_rows, mix_lambda, head_gain, head_index):
    kv_index = head_index // (HEADS // KV_HEADS)
    head_query = lax.dynamic_slice_in_dim(query_maps, (head_index * 2 * HD).astype(jnp.int32), 2 * HD, 1)
    head_key = lax.dynamic_slice_in_dim(key_maps, (kv_index * 2 * HD).astype(jnp.int32), 2 * HD, 1)
    head_value = lax.dynamic_slice_in_dim(value_rows, (kv_index * VD).astype(jnp.int32), VD, 1)
    head_lambda = mix_lambda[head_index]
    score_scale = HD ** (-0.5)
    block_rows = math.gcd(SEQ, 512)
    query_blocks = head_query.reshape(SEQ // block_rows, block_rows, 2 * HD)

    def weighted(scores):
        row_max = lax.optimization_barrier(jnp.max(scores, axis=1, keepdims=True))
        exp_scores = jnp.exp(scores - row_max)
        row_total = lax.optimization_barrier(jnp.sum(exp_scores, axis=1, keepdims=True))
        return jnp.dot(exp_scores.astype(jnp.bfloat16), head_value, preferred_element_type=jnp.float32) / row_total

    def one_block(query_block):
        first_map = jnp.dot(query_block[:, :HD], head_key[:, :HD].T, preferred_element_type=jnp.float32) * score_scale
        second_map = jnp.dot(query_block[:, HD:], head_key[:, HD:].T, preferred_element_type=jnp.float32) * score_scale
        difference = weighted(first_map) - head_lambda * weighted(second_map)
        inverse_rms = lax.rsqrt(lax.optimization_barrier(jnp.mean(difference * difference, axis=1, keepdims=True)) + norm_eps)
        return (difference * inverse_rms * head_gain).astype(jnp.bfloat16)
    return lax.map(one_block, query_blocks).reshape(SEQ, VD)

def reference(query_maps, key_maps, value_rows, mix_lambda, head_gain, out_weight, residual, norm_gain, routes, route_weight, expert_gate, expert_up, expert_down, shared_gate, shared_up, shared_down):

    def per_head(head_index):
        return head_attention(query_maps, key_maps, value_rows, mix_lambda, head_gain, head_index)
    attended = lax.map(per_head, jnp.arange(HEADS, dtype=jnp.int32))
    attended = jnp.transpose(attended, (1, 0, 2)).reshape(SEQ, HEADS * VD)
    projected = jnp.dot(attended, out_weight, preferred_element_type=jnp.float32)
    stream = (residual.astype(jnp.float32) + projected).astype(jnp.bfloat16)
    stream_wide = stream.astype(jnp.float32)
    inverse_rms = lax.rsqrt(lax.optimization_barrier(jnp.mean(stream_wide * stream_wide, axis=1, keepdims=True)) + norm_eps)
    normed = (stream_wide * inverse_rms * norm_gain).astype(jnp.bfloat16)
    blocks = SEQ // ROWS_DEV
    flat_routes, slot_index = jax.vmap(slot_targets)(routes.reshape(blocks, ROWS_DEV, TOP_K))
    expert_row = jnp.arange(blocks, dtype=jnp.int32)[:, None] * CAP + slot_index
    assignment = jnp.arange(SEQ * TOP_K, dtype=jnp.int32).reshape(blocks, ROWS_DEV * TOP_K)
    holder = jnp.full((EXPERTS, blocks * CAP), SEQ * TOP_K, jnp.int32).at[flat_routes, expert_row].set(assignment)
    padded_tokens = jnp.concatenate([normed, jnp.zeros((1, D), jnp.bfloat16)], axis=0)
    padded_weights = jnp.concatenate([route_weight.reshape(-1), jnp.zeros((1,), jnp.float32)], axis=0)

    def expert_step(running, inputs):
        holder_row, gate_weight, up_weight, down_weight = inputs
        token_index = holder_row // TOP_K
        outputs = grouped_feedforward(padded_tokens[token_index], gate_weight, up_weight, down_weight)
        contribution = padded_weights[holder_row][:, None] * outputs.astype(jnp.float32)
        return (running.at[token_index].add(contribution), None)
    routed_total = lax.scan(expert_step, jnp.zeros((SEQ + 1, D), jnp.float32), (holder, expert_gate, expert_up, expert_down))[0]
    shared_out = grouped_feedforward(normed, shared_gate, shared_up, shared_down)
    return (stream_wide + shared_out.astype(jnp.float32) + routed_total[:SEQ]).astype(jnp.bfloat16)
```

```python
from functools import partial

import jax
import jax.numpy as jnp
from jax import lax
from jax.experimental import pallas as pl
from jax.experimental.pallas import tpu as pltpu
from jax.sharding import PartitionSpec as P

norm_eps = 1e-06
lowest_score = -1e30


def slot_targets(block_routes, experts, capacity):
    flat_routes = block_routes.reshape(-1)
    onehot = (flat_routes[:, None] == jnp.arange(experts, dtype=jnp.int32)[None, :]).astype(
        jnp.int32
    )
    earlier = jnp.cumsum(onehot, axis=0) - onehot
    return flat_routes * capacity + jnp.sum(earlier * onehot, axis=1)


def build_buffer(token_rows, block_routes, experts, capacity):
    targets = slot_targets(block_routes, experts, capacity)
    row_total = block_routes.shape[0]
    route_count = block_routes.shape[1]
    source_row = jnp.arange(row_total * route_count, dtype=jnp.int32) // route_count
    holder = jnp.full((experts * capacity,), row_total, jnp.int32).at[targets].set(source_row)
    padded = jnp.concatenate(
        [token_rows, jnp.zeros((1, token_rows.shape[1]), token_rows.dtype)], axis=0
    )
    return (padded[holder], targets)


def attention_block(carried, queries, key_block, value_block, score_scale):
    run_max, run_sum, accumulated = carried
    kv_local = run_max.shape[0]
    key_heads = key_block.reshape(key_block.shape[0], kv_local, 2, -1)
    value_heads = value_block.reshape(value_block.shape[0], kv_local, -1)
    scores = (
        jnp.einsum("qagcd,racd->agcqr", queries, key_heads, preferred_element_type=jnp.float32)
        * score_scale
    )
    new_max = jnp.maximum(run_max, jnp.max(scores, axis=-1))
    rescale = jnp.exp(run_max - new_max)
    weights = jnp.exp(scores - new_max[..., None])
    run_sum = run_sum * rescale + jnp.sum(weights, axis=-1)
    update = jnp.einsum(
        "agcqr,rae->agcqe",
        weights.astype(jnp.bfloat16),
        value_heads,
        preferred_element_type=jnp.float32,
    )
    return (new_max, run_sum, accumulated * rescale[..., None] + update)


def fold_keys(carried, pieces, first_row, queries, score_scale):
    key_piece, value_piece = pieces
    total_rows = key_piece.shape[0]
    block_rows = total_rows
    for candidate in (2048, 1024, 512):
        if total_rows % candidate == 0:
            block_rows = candidate
            break
    block_count = total_rows // block_rows

    def block_step(block_index, running):
        start_row = block_index * block_rows
        return attention_block(
            running,
            queries,
            lax.dynamic_slice_in_dim(key_piece, start_row, block_rows, 0),
            lax.dynamic_slice_in_dim(value_piece, start_row, block_rows, 0),
            score_scale,
        )

    return lax.fori_loop(0, block_count, block_step, carried)


def whole_experts(arrived, whole_gate, whole_up, whole_down, senders, capacity, groups):
    local_experts = whole_gate.shape[0]
    width = arrived.shape[-1]
    rows_in = arrived.reshape(senders, local_experts, capacity, width)
    gate_value = jnp.einsum(
        "sjtd,jdf->sjtf", rows_in, whole_gate, preferred_element_type=jnp.float32
    )
    up_value = jnp.einsum("sjtd,jdf->sjtf", rows_in, whole_up, preferred_element_type=jnp.float32)
    hidden = (jax.nn.silu(gate_value) * up_value).astype(jnp.bfloat16)
    hidden_units = hidden.shape[-1]
    hidden = hidden.reshape(senders, local_experts, capacity, groups, hidden_units // groups)
    down_groups = whole_down.reshape(local_experts, groups, hidden_units // groups, width)
    group_sums = jnp.einsum(
        "sjtgf,jgfd->sjtgd", hidden, down_groups, preferred_element_type=jnp.float32
    )
    group_sums = lax.optimization_barrier(group_sums.astype(jnp.bfloat16)).astype(jnp.float32)
    return (
        jnp.sum(group_sums, axis=3)
        .astype(jnp.bfloat16)
        .reshape(senders * local_experts * capacity, width)
    )


def body(
    query_maps,
    key_maps,
    value_rows,
    mix_lambda,
    head_gain,
    out_weight,
    residual,
    norm_gain,
    routes,
    route_weight,
    expert_gate,
    expert_up,
    expert_down,
    shared_gate,
    shared_up,
    shared_down,
):
    local_heads = mix_lambda.shape[0]
    head_width = head_gain.shape[0]
    kv_local = value_rows.shape[1] // head_width
    head_group = local_heads // kv_local
    head_dim = key_maps.shape[1] // (2 * kv_local)
    token_count = query_maps.shape[0]
    queries = query_maps.reshape(token_count, kv_local, head_group, 2, head_dim)
    start_max = jnp.full((kv_local, head_group, 2, token_count), lowest_score, jnp.float32)
    start_sum = jnp.zeros((kv_local, head_group, 2, token_count), jnp.float32)
    start_values = jnp.zeros((kv_local, head_group, 2, token_count, head_width), jnp.float32)
    folder = partial(fold_keys, queries=queries, score_scale=head_dim ** (-0.5))
    run_max, run_sum, accumulated = folder(
        (start_max, start_sum, start_values),
        (
            lax.all_gather(key_maps, "sp", axis=0, tiled=True),
            lax.all_gather(value_rows, "sp", axis=0, tiled=True),
        ),
        jnp.int32(0),
    )
    normalized = accumulated / run_sum[..., None]
    lambdas = mix_lambda.reshape(kv_local, head_group, 1, 1)
    difference = normalized[:, :, 0] - lambdas * normalized[:, :, 1]
    inverse_rms = lax.rsqrt(jnp.mean(difference * difference, axis=-1, keepdims=True) + norm_eps)
    head_scaled = (difference * inverse_rms * head_gain).astype(jnp.bfloat16)
    attended = jnp.transpose(head_scaled, (2, 0, 1, 3)).reshape(
        token_count, local_heads * head_width
    )
    columns = lax.axis_size("tp")
    column = lax.axis_index("tp")
    rows_dev = token_count // columns
    own_rows = lax.dynamic_slice_in_dim(
        out_weight, column * attended.shape[1], attended.shape[1], 0
    )
    projected = lax.psum_scatter(
        jnp.dot(attended, own_rows, preferred_element_type=jnp.float32).astype(jnp.bfloat16),
        "tp",
        scatter_dimension=0,
        tiled=True,
    ).astype(jnp.float32)
    stream = (residual.astype(jnp.float32) + projected).astype(jnp.bfloat16)
    stream_wide = stream.astype(jnp.float32)
    stream_rms = lax.rsqrt(jnp.mean(stream_wide * stream_wide, axis=1, keepdims=True) + norm_eps)
    normed = (stream_wide * stream_rms * norm_gain).astype(jnp.bfloat16)
    senders = lax.axis_size("sp")
    local_experts = expert_gate.shape[0]
    experts = senders * local_experts
    route_count = routes.shape[1]
    capacity = max(2, 2 * rows_dev * route_count // experts)
    local_routed = None
    whole_gate, whole_up, whole_down = (
        lax.all_gather(expert_gate, "tp", axis=2, tiled=True),
        lax.all_gather(expert_up, "tp", axis=2, tiled=True),
        lax.all_gather(expert_down, "tp", axis=1, tiled=True),
    )
    own_routes = lax.dynamic_slice_in_dim(routes, column * rows_dev, rows_dev, 0)
    buffer, targets = build_buffer(normed, own_routes, experts, capacity)
    arrived = lax.all_to_all(buffer, "sp", split_axis=0, concat_axis=0, tiled=True)
    local_routed = whole_experts(
        arrived, whole_gate, whole_up, whole_down, senders, capacity, columns
    )
    shared_rows = lax.all_gather(normed[None], "tp", axis=0, tiled=True)
    shared_in = shared_rows
    shared_in = shared_in.reshape(1 * lax.axis_size("tp") * rows_dev, shared_in.shape[-1])
    shared_hidden = (
        jax.nn.silu(jnp.dot(shared_in, shared_gate, preferred_element_type=jnp.float32))
        * jnp.dot(shared_in, shared_up, preferred_element_type=jnp.float32)
    ).astype(jnp.bfloat16)
    shared_out = jnp.dot(shared_hidden, shared_down, preferred_element_type=jnp.float32)
    pieces = shared_out.reshape(1 * lax.axis_size("tp"), rows_dev, shared_out.shape[-1])
    terms_out = pieces.astype(jnp.bfloat16)
    summed = (
        lax.psum_scatter(
            lax.optimization_barrier(terms_out).astype(jnp.float32).astype(jnp.bfloat16),
            "tp",
            scatter_dimension=0,
            tiled=True,
        )
        .astype(jnp.float32)[0]
        .astype(jnp.bfloat16)
    )
    returned = lax.all_to_all(local_routed, "sp", split_axis=0, concat_axis=0, tiled=True)
    picked = (
        returned[targets].reshape(rows_dev, route_count, returned.shape[-1]).astype(jnp.float32)
    )
    routed_sum = jnp.sum(route_weight[:, :, None] * picked, axis=1)
    return (stream_wide + summed.astype(jnp.float32) + routed_sum).astype(jnp.bfloat16)


MESH = pl.DeviceIdType.MESH


def peer_barrier(peers):
    barrier = pltpu.get_barrier_semaphore()
    for peer in peers:
        pl.semaphore_signal(barrier, inc=1, device_id=peer, device_id_type=MESH)
    pl.semaphore_wait(barrier, len(peers))


def remote(src, dst, send_sem, recv_sem, peer):
    return pltpu.make_async_remote_copy(
        src_ref=src,
        dst_ref=dst,
        send_sem=send_sem,
        recv_sem=recv_sem,
        device_id=peer,
        device_id_type=MESH,
    )


def grid_place(sp):
    s = lax.axis_index("sp")
    t = lax.axis_index("tp")
    return s, t, s // 2, s % 2, sp // 2


def gather_kernel(sp, tp, count, with_tp, *refs):
    ins, refs = refs[:count], refs[count:]
    outs, refs = refs[:count], refs[count:]
    if with_tp:
        tp_out, refs = refs[0], refs[1:]
    send_sem, recv_sem, local_sem = refs[:3]
    s, t, z, x, depth = grid_place(sp)
    line = [(lax.rem(z + k, depth) * 2 + x, t) for k in range(1, depth)]
    across = (z * 2 + (1 - x), t)
    columns = [(s, lax.rem(t + k, tp)) for k in range(1, tp)] if with_tp else []
    peer_barrier(line + [across] + columns)
    copies = []
    arrivals = []
    for i in range(count):
        for k in range(depth - 1, 0, -1):
            copy = remote(
                ins[i], outs[i].at[s], send_sem.at[i, k], recv_sem.at[i, k], line[k - 1]
            )
            copy.start()
            copies.append(copy)
            arrivals.append((k, i, copy))
    for i in range(count):
        copy = remote(
            ins[i], outs[i].at[s], send_sem.at[i, depth], recv_sem.at[i, depth], across
        )
        copy.start()
        copies.append(copy)
    side = []
    if with_tp:
        for k in range(1, tp):
            copy = remote(
                ins[0],
                tp_out.at[t],
                send_sem.at[0, 2 * depth + k],
                recv_sem.at[0, 2 * depth + k],
                columns[k - 1],
            )
            copy.start()
            side.append(copy)
        own = pltpu.make_async_copy(ins[0], tp_out.at[t], local_sem.at[count])
        own.start()
    locals_ = []
    for i in range(count):
        copy = pltpu.make_async_copy(ins[i], outs[i].at[s], local_sem.at[i])
        copy.start()
        locals_.append(copy)
    order = {1: 0, 3: 1, 2: 2}
    arrivals.sort(key=lambda item: (order.get(item[0], item[0]), item[1]))
    for k, i, copy in arrivals:
        copy.wait_recv()
        origin = lax.rem(z + depth - k, depth) * 2 + x
        relay = remote(
            outs[i].at[origin],
            outs[i].at[origin],
            send_sem.at[i, depth + k],
            recv_sem.at[i, depth + k],
            across,
        )
        relay.start()
        side.append(relay)
    for _, _, copy in arrivals:
        copy.wait_send()
    for copy in copies:
        if not any(copy is entry[2] for entry in arrivals):
            copy.wait()
    for copy in side:
        copy.wait()
    for copy in locals_:
        copy.wait()
    if with_tp:
        own.wait()


def gather_sp(arrays, sp, tp, with_tp, collective_id):
    count = len(arrays)
    depth = sp // 2
    shapes = [jax.ShapeDtypeStruct((sp,) + a.shape, a.dtype) for a in arrays]
    if with_tp:
        shapes.append(jax.ShapeDtypeStruct((tp,) + arrays[0].shape, arrays[0].dtype))
    slots = 2 * depth + tp
    return pl.pallas_call(
        partial(gather_kernel, sp, tp, count, with_tp),
        out_shape=tuple(shapes),
        in_specs=[pl.BlockSpec(memory_space=pltpu.VMEM)] * count,
        out_specs=tuple([pl.BlockSpec(memory_space=pltpu.VMEM)] * len(shapes)),
        scratch_shapes=[
            pltpu.SemaphoreType.DMA((count, slots)),
            pltpu.SemaphoreType.DMA((count, slots)),
            pltpu.SemaphoreType.DMA((count + 1,)),
        ],
        compiler_params=pltpu.CompilerParams(
            collective_id=collective_id, has_side_effects=True
        ),
        cost_estimate=pl.CostEstimate(flops=0, bytes_accessed=40_000_000, transcendentals=0),
    )(*arrays)


def heads_kernel(tp, x_ref, out_ref, send_sem, recv_sem, local_sem):
    s = lax.axis_index("sp")
    t = lax.axis_index("tp")
    rows = out_ref.shape[0]
    width = x_ref.shape[1]
    peers = [(s, lax.rem(t + k, tp)) for k in range(1, tp)]
    peer_barrier(peers)
    mine = pl.ds(pl.multiple_of(t * width, width), width)
    copies = []
    for k in range(1, tp):
        target = lax.rem(t + k, tp)
        copy = remote(
            x_ref.at[pl.ds(pl.multiple_of(target * rows, rows), rows)],
            out_ref.at[:, mine],
            send_sem.at[k],
            recv_sem.at[k],
            peers[k - 1],
        )
        copy.start()
        copies.append(copy)
    own = pltpu.make_async_copy(
        x_ref.at[pl.ds(pl.multiple_of(t * rows, rows), rows)], out_ref.at[:, mine], local_sem
    )
    own.start()
    for copy in copies:
        copy.wait()
    own.wait()


def exchange_heads(attended, tp, collective_id):
    tokens, width = attended.shape
    return pl.pallas_call(
        partial(heads_kernel, tp),
        out_shape=jax.ShapeDtypeStruct((tokens // tp, tp * width), attended.dtype),
        in_specs=[pl.BlockSpec(memory_space=pltpu.VMEM)],
        out_specs=pl.BlockSpec(memory_space=pltpu.VMEM),
        scratch_shapes=[
            pltpu.SemaphoreType.DMA((tp,)),
            pltpu.SemaphoreType.DMA((tp,)),
            pltpu.SemaphoreType.DMA,
        ],
        compiler_params=pltpu.CompilerParams(
            collective_id=collective_id, has_side_effects=True
        ),
        cost_estimate=pl.CostEstimate(flops=0, bytes_accessed=10_000_000, transcendentals=0),
    )(attended)


def return_kernel(
    sp,
    tp,
    routed_ref,
    shared_ref,
    stream_ref,
    out_ref,
    from_across,
    pair_sum,
    from_line,
    from_column,
    send_sem,
    recv_sem,
):
    s, t, z, x, depth = grid_place(sp)
    line = [(lax.rem(z + k, depth) * 2 + x, t) for k in range(1, depth)]
    across = (z * 2 + (1 - x), t)
    columns = [(s, lax.rem(t + k, tp)) for k in range(1, tp)]
    peer_barrier(line + [across] + columns)
    order = [2, 3, 1] if depth == 4 else list(range(1, depth))
    crossing = {}
    for k in order + [0]:
        target = lax.rem(z + k, depth) * 2 + (1 - x)
        copy = remote(
            routed_ref.at[target], from_across.at[k], send_sem.at[k], recv_sem.at[k], across
        )
        copy.start()
        crossing[k] = copy
    side = []
    for k in range(1, tp):
        copy = remote(
            shared_ref.at[lax.rem(t + k, tp)],
            from_column.at[k - 1],
            send_sem.at[2 * depth + k],
            recv_sem.at[2 * depth + k],
            columns[k - 1],
        )
        copy.start()
        side.append(copy)
    moving = []
    for k in order:
        crossing[k].wait_recv()
        target = lax.rem(z + k, depth) * 2 + x
        pair_sum[k - 1] = (
            routed_ref[target].astype(jnp.float32) + from_across[k].astype(jnp.float32)
        ).astype(jnp.bfloat16)
        copy = remote(
            pair_sum.at[k - 1],
            from_line.at[k - 1],
            send_sem.at[depth + k],
            recv_sem.at[depth + k],
            line[k - 1],
        )
        copy.start()
        moving.append(copy)
    total = stream_ref[...].astype(jnp.float32) + shared_ref[t].astype(jnp.float32)
    for k, copy in enumerate(side):
        copy.wait_recv()
        total = total + from_column[k].astype(jnp.float32)
    crossing[0].wait_recv()
    total = total + routed_ref[s].astype(jnp.float32) + from_across[0].astype(jnp.float32)
    for k, copy in zip(order, moving):
        copy.wait_recv()
        total = total + from_line[k - 1].astype(jnp.float32)
    out_ref[...] = total.astype(out_ref.dtype)
    for copy in list(crossing.values()) + side + moving:
        copy.wait_send()


def return_rows(routed, shared, stream, sp, tp, collective_id):
    rows, width = stream.shape
    depth = sp // 2
    slots = 2 * depth + tp
    return pl.pallas_call(
        partial(return_kernel, sp, tp),
        out_shape=jax.ShapeDtypeStruct((rows, width), jnp.bfloat16),
        in_specs=[pl.BlockSpec(memory_space=pltpu.VMEM)] * 3,
        out_specs=pl.BlockSpec(memory_space=pltpu.VMEM),
        scratch_shapes=[
            pltpu.VMEM((depth, rows, width), jnp.bfloat16),
            pltpu.VMEM((depth - 1, rows, width), jnp.bfloat16),
            pltpu.VMEM((depth - 1, rows, width), jnp.bfloat16),
            pltpu.VMEM((tp - 1, rows, width), jnp.bfloat16),
            pltpu.SemaphoreType.DMA((slots,)),
            pltpu.SemaphoreType.DMA((slots,)),
        ],
        compiler_params=pltpu.CompilerParams(
            collective_id=collective_id, has_side_effects=True
        ),
        cost_estimate=pl.CostEstimate(flops=0, bytes_accessed=60_000_000, transcendentals=0),
    )(routed, shared, stream)


def experts_kernel(groups, *refs):
    rows_ref, weight_ref = refs[:2]
    triples = [refs[2 + 3 * q : 5 + 3 * q] for q in range(groups)]
    out_ref, gate_buf, up_buf, down_buf, total, sems = refs[2 + 3 * groups :]
    copies = []
    for q in range(groups):
        for n, (source, buffer) in enumerate(zip(triples[q], (gate_buf, up_buf, down_buf))):
            copy = pltpu.make_async_copy(source, buffer.at[q], sems.at[q, n])
            copy.start()
            copies.append(copy)
    for q in range(groups):
        copies[3 * q].wait()
        gate_value = jnp.dot(rows_ref[...], gate_buf[q], preferred_element_type=jnp.float32)
        copies[3 * q + 1].wait()
        up_value = jnp.dot(rows_ref[...], up_buf[q], preferred_element_type=jnp.float32)
        hidden = (jax.nn.silu(gate_value) * up_value).astype(jnp.bfloat16)
        copies[3 * q + 2].wait()
        product = jnp.dot(hidden, down_buf[q], preferred_element_type=jnp.float32)
        if q == 0:
            total[...] = product
        elif q < groups - 1:
            total[...] += product
        else:
            out_ref[...] = ((total[...] + product) * weight_ref[...]).astype(jnp.bfloat16)


def run_experts(rows_in, dense_weight, triples):
    groups = len(triples)
    count, width = rows_in.shape
    units = triples[0][0].shape[1]
    flat = [array for triple in triples for array in triple]
    return pl.pallas_call(
        partial(experts_kernel, groups),
        out_shape=jax.ShapeDtypeStruct((count, width), jnp.bfloat16),
        in_specs=[pl.BlockSpec(memory_space=pltpu.VMEM)] * 2
        + [pl.BlockSpec(memory_space=pl.ANY)] * len(flat),
        out_specs=pl.BlockSpec(memory_space=pltpu.VMEM),
        scratch_shapes=[
            pltpu.VMEM((groups, width, units), jnp.bfloat16),
            pltpu.VMEM((groups, width, units), jnp.bfloat16),
            pltpu.VMEM((groups, units, width), jnp.bfloat16),
            pltpu.VMEM((count, width), jnp.float32),
            pltpu.SemaphoreType.DMA((groups, 3)),
        ],
        compiler_params=pltpu.CompilerParams(vmem_limit_bytes=40 * 1024 * 1024),
        cost_estimate=pl.CostEstimate(
            flops=6 * count * width * units * groups,
            bytes_accessed=12_000_000,
            transcendentals=0,
        ),
    )(rows_in, dense_weight, *flat)


def dense_body(
    query_maps,
    key_maps,
    value_rows,
    mix_lambda,
    head_gain,
    out_weight,
    residual,
    norm_gain,
    routes,
    route_weight,
    expert_gate,
    expert_up,
    expert_down,
    shared_gate,
    shared_up,
    shared_down,
):
    sp = lax.axis_size("sp")
    tp = lax.axis_size("tp")
    s = lax.axis_index("sp")
    t = lax.axis_index("tp")

    def swapped(array, step):
        return lax.ppermute(array, "tp", [(i, i ^ step) for i in range(tp)])

    own = (expert_gate[0], expert_up[0], expert_down[0])
    far = tuple(swapped(a, 2) for a in own)
    near = tuple(swapped(a, 1) for a in own)
    near_far = tuple(swapped(a, 1) for a in far)

    local_heads = mix_lambda.shape[0]
    head_width = head_gain.shape[0]
    kv_local = value_rows.shape[1] // head_width
    head_group = local_heads // kv_local
    head_dim = key_maps.shape[1] // (2 * kv_local)
    token_count = query_maps.shape[0]
    rows_dev = token_count // tp
    experts = sp

    own_routes = lax.dynamic_slice_in_dim(routes, t * rows_dev, rows_dev, 0)
    named = own_routes[None, :, :] == jnp.arange(experts, dtype=jnp.int32)[:, None, None]
    table = jnp.sum(jnp.where(named, route_weight[None], 0.0), axis=2)
    lanes = -(-rows_dev // 128) * 128
    table = jnp.pad(table, ((0, 0), (0, lanes - rows_dev)))

    key_all, value_all, tables = gather_sp([key_maps, value_rows, table], sp, tp, False, 1)
    key_all = key_all.reshape(sp * token_count, -1)
    value_all = value_all.reshape(sp * token_count, -1)
    dense_weight = lax.dynamic_index_in_dim(tables, s, 1, False)[:, :rows_dev]
    dense_weight = dense_weight.reshape(sp * rows_dev, 1)

    queries = query_maps.reshape(token_count, kv_local, head_group, 2, head_dim)
    start_max = jnp.full((kv_local, head_group, 2, token_count), lowest_score, jnp.float32)
    start_sum = jnp.zeros((kv_local, head_group, 2, token_count), jnp.float32)
    start_values = jnp.zeros((kv_local, head_group, 2, token_count, head_width), jnp.float32)
    run_max, run_sum, accumulated = fold_keys(
        (start_max, start_sum, start_values),
        (key_all, value_all),
        jnp.int32(0),
        queries,
        head_dim ** (-0.5),
    )
    normalized = accumulated / run_sum[..., None]
    lambdas = mix_lambda.reshape(kv_local, head_group, 1, 1)
    difference = normalized[:, :, 0] - lambdas * normalized[:, :, 1]
    inverse_rms = lax.rsqrt(jnp.mean(difference * difference, axis=-1, keepdims=True) + norm_eps)
    head_scaled = (difference * inverse_rms * head_gain).astype(jnp.bfloat16)
    attended = jnp.transpose(head_scaled, (2, 0, 1, 3)).reshape(
        token_count, local_heads * head_width
    )
    attended = exchange_heads(attended, tp, 2)
    projected = jnp.dot(attended, out_weight, preferred_element_type=jnp.float32)
    stream = (residual.astype(jnp.float32) + projected).astype(jnp.bfloat16)
    stream_wide = stream.astype(jnp.float32)
    stream_rms = lax.rsqrt(jnp.mean(stream_wide * stream_wide, axis=1, keepdims=True) + norm_eps)
    normed = (stream_wide * stream_rms * norm_gain).astype(jnp.bfloat16)

    routed_in, shared_in = gather_sp([normed], sp, tp, True, 3)
    width = normed.shape[1]
    shared_in = shared_in.reshape(tp * rows_dev, width)
    shared_hidden = (
        jax.nn.silu(jnp.dot(shared_in, shared_gate, preferred_element_type=jnp.float32))
        * jnp.dot(shared_in, shared_up, preferred_element_type=jnp.float32)
    ).astype(jnp.bfloat16)
    shared_out = jnp.dot(shared_hidden, shared_down, preferred_element_type=jnp.float32)
    shared_out = shared_out.astype(jnp.bfloat16).reshape(tp, rows_dev, width)

    routed = run_experts(
        routed_in.reshape(sp * rows_dev, width), dense_weight, (own, near, far, near_far)
    )
    return return_rows(routed.reshape(sp, rows_dev, width), shared_out, stream, sp, tp, 4)


def solution(mesh):
    in_specs = (
        P("sp", "tp"),
        P("sp", "tp"),
        P("sp", "tp"),
        P("tp"),
        P(),
        P(),
        P(("sp", "tp"), None),
        P(),
        P("sp", None),
        P(("sp", "tp"), None),
        P("sp", None, "tp"),
        P("sp", None, "tp"),
        P("sp", "tp", None),
        P(None, "tp"),
        P(None, "tp"),
        P("tp", None),
    )
    out_specs = P(("sp", "tp"), None)
    sp, tp = mesh.shape["sp"], mesh.shape["tp"]

    def chosen(*args):
        route_count = args[8].shape[1]
        experts = sp * args[10].shape[0]
        rows_dev = args[6].shape[0]
        whole_blocks = 2 * rows_dev * route_count >= experts * rows_dev
        dense = whole_blocks and args[10].shape[0] == 1 and sp == 8 and tp == 4
        return (dense_body if dense else body)(*args)

    return jax.shard_map(
        chosen, mesh=mesh, in_specs=in_specs, out_specs=out_specs, check_vma=False
    )
```

```python
from functools import partial

import jax
import jax.numpy as jnp
from jax import lax
from jax.experimental import pallas as pl
from jax.experimental.pallas import tpu as pltpu
from jax.sharding import PartitionSpec as P


norm_eps = 1e-06
lowest_score = -1e30


def slot_targets(block_routes, experts, capacity):
    flat_routes = block_routes.reshape(-1)
    onehot = (flat_routes[:, None] == jnp.arange(experts, dtype=jnp.int32)[None, :]).astype(
        jnp.int32
    )
    earlier = jnp.cumsum(onehot, axis=0) - onehot
    return flat_routes * capacity + jnp.sum(earlier * onehot, axis=1)


def build_buffer(token_rows, block_routes, experts, capacity):
    targets = slot_targets(block_routes, experts, capacity)
    row_total = block_routes.shape[0]
    route_count = block_routes.shape[1]
    source_row = jnp.arange(row_total * route_count, dtype=jnp.int32) // route_count
    holder = jnp.full((experts * capacity,), row_total, jnp.int32).at[targets].set(source_row)
    padded = jnp.concatenate(
        [token_rows, jnp.zeros((1, token_rows.shape[1]), token_rows.dtype)], axis=0
    )
    return (padded[holder], targets)


def attention_block(carried, queries, key_block, value_block, score_scale):
    run_max, run_sum, accumulated = carried
    kv_local = run_max.shape[0]
    key_heads = key_block.reshape(key_block.shape[0], kv_local, 2, -1)
    value_heads = value_block.reshape(value_block.shape[0], kv_local, -1)
    scores = (
        jnp.einsum("qagcd,racd->agcqr", queries, key_heads, preferred_element_type=jnp.float32)
        * score_scale
    )
    new_max = jnp.maximum(run_max, jnp.max(scores, axis=-1))
    rescale = jnp.exp(run_max - new_max)
    weights = jnp.exp(scores - new_max[..., None])
    run_sum = run_sum * rescale + jnp.sum(weights, axis=-1)
    update = jnp.einsum(
        "agcqr,rae->agcqe",
        weights.astype(jnp.bfloat16),
        value_heads,
        preferred_element_type=jnp.float32,
    )
    return (new_max, run_sum, accumulated * rescale[..., None] + update)


def fold_keys(carried, pieces, first_row, queries, score_scale):
    key_piece, value_piece = pieces
    total_rows = key_piece.shape[0]
    block_rows = total_rows
    for candidate in (2048, 1024, 512):
        if total_rows % candidate == 0:
            block_rows = candidate
            break
    block_count = total_rows // block_rows

    def block_step(block_index, running):
        start_row = block_index * block_rows
        return attention_block(
            running,
            queries,
            lax.dynamic_slice_in_dim(key_piece, start_row, block_rows, 0),
            lax.dynamic_slice_in_dim(value_piece, start_row, block_rows, 0),
            score_scale,
        )

    return lax.fori_loop(0, block_count, block_step, carried)


def whole_experts(arrived, whole_gate, whole_up, whole_down, senders, capacity, groups):
    local_experts = whole_gate.shape[0]
    width = arrived.shape[-1]
    rows_in = arrived.reshape(senders, local_experts, capacity, width)
    gate_value = jnp.einsum(
        "sjtd,jdf->sjtf", rows_in, whole_gate, preferred_element_type=jnp.float32
    )
    up_value = jnp.einsum("sjtd,jdf->sjtf", rows_in, whole_up, preferred_element_type=jnp.float32)
    hidden = (jax.nn.silu(gate_value) * up_value).astype(jnp.bfloat16)
    hidden_units = hidden.shape[-1]
    hidden = hidden.reshape(senders, local_experts, capacity, groups, hidden_units // groups)
    down_groups = whole_down.reshape(local_experts, groups, hidden_units // groups, width)
    group_sums = jnp.einsum(
        "sjtgf,jgfd->sjtgd", hidden, down_groups, preferred_element_type=jnp.float32
    )
    group_sums = lax.optimization_barrier(group_sums.astype(jnp.bfloat16)).astype(jnp.float32)
    return (
        jnp.sum(group_sums, axis=3)
        .astype(jnp.bfloat16)
        .reshape(senders * local_experts * capacity, width)
    )


def body(
    query_maps,
    key_maps,
    value_rows,
    mix_lambda,
    head_gain,
    out_weight,
    residual,
    norm_gain,
    routes,
    route_weight,
    expert_gate,
    expert_up,
    expert_down,
    shared_gate,
    shared_up,
    shared_down,
):
    local_heads = mix_lambda.shape[0]
    head_width = head_gain.shape[0]
    kv_local = value_rows.shape[1] // head_width
    head_group = local_heads // kv_local
    head_dim = key_maps.shape[1] // (2 * kv_local)
    token_count = query_maps.shape[0]
    queries = query_maps.reshape(token_count, kv_local, head_group, 2, head_dim)
    start_max = jnp.full((kv_local, head_group, 2, token_count), lowest_score, jnp.float32)
    start_sum = jnp.zeros((kv_local, head_group, 2, token_count), jnp.float32)
    start_values = jnp.zeros((kv_local, head_group, 2, token_count, head_width), jnp.float32)
    folder = partial(fold_keys, queries=queries, score_scale=head_dim ** (-0.5))
    _, run_sum, accumulated = folder(
        (start_max, start_sum, start_values),
        (
            lax.all_gather(key_maps, "sp", axis=0, tiled=True),
            lax.all_gather(value_rows, "sp", axis=0, tiled=True),
        ),
        jnp.int32(0),
    )
    normalized = accumulated / run_sum[..., None]
    lambdas = mix_lambda.reshape(kv_local, head_group, 1, 1)
    difference = normalized[:, :, 0] - lambdas * normalized[:, :, 1]
    inverse_rms = lax.rsqrt(jnp.mean(difference * difference, axis=-1, keepdims=True) + norm_eps)
    head_scaled = (difference * inverse_rms * head_gain).astype(jnp.bfloat16)
    attended = jnp.transpose(head_scaled, (2, 0, 1, 3)).reshape(
        token_count, local_heads * head_width
    )
    columns = lax.axis_size("tp")
    column = lax.axis_index("tp")
    rows_dev = token_count // columns
    own_rows = lax.dynamic_slice_in_dim(
        out_weight, column * attended.shape[1], attended.shape[1], 0
    )
    projected = lax.psum_scatter(
        jnp.dot(attended, own_rows, preferred_element_type=jnp.float32).astype(jnp.bfloat16),
        "tp",
        scatter_dimension=0,
        tiled=True,
    ).astype(jnp.float32)
    stream = (residual.astype(jnp.float32) + projected).astype(jnp.bfloat16)
    stream_wide = stream.astype(jnp.float32)
    stream_rms = lax.rsqrt(jnp.mean(stream_wide * stream_wide, axis=1, keepdims=True) + norm_eps)
    normed = (stream_wide * stream_rms * norm_gain).astype(jnp.bfloat16)
    senders = lax.axis_size("sp")
    local_experts = expert_gate.shape[0]
    experts = senders * local_experts
    route_count = routes.shape[1]
    capacity = max(2, 2 * rows_dev * route_count // experts)
    local_routed = None
    whole_gate, whole_up, whole_down = (
        lax.all_gather(expert_gate, "tp", axis=2, tiled=True),
        lax.all_gather(expert_up, "tp", axis=2, tiled=True),
        lax.all_gather(expert_down, "tp", axis=1, tiled=True),
    )
    own_routes = lax.dynamic_slice_in_dim(routes, column * rows_dev, rows_dev, 0)
    buffer, targets = build_buffer(normed, own_routes, experts, capacity)
    arrived = lax.all_to_all(buffer, "sp", split_axis=0, concat_axis=0, tiled=True)
    local_routed = whole_experts(
        arrived, whole_gate, whole_up, whole_down, senders, capacity, columns
    )
    shared_rows = lax.all_gather(normed[None], "tp", axis=0, tiled=True)
    shared_in = shared_rows
    shared_in = shared_in.reshape(1 * lax.axis_size("tp") * rows_dev, shared_in.shape[-1])
    shared_hidden = (
        jax.nn.silu(jnp.dot(shared_in, shared_gate, preferred_element_type=jnp.float32))
        * jnp.dot(shared_in, shared_up, preferred_element_type=jnp.float32)
    ).astype(jnp.bfloat16)
    shared_out = jnp.dot(shared_hidden, shared_down, preferred_element_type=jnp.float32)
    pieces = shared_out.reshape(1 * lax.axis_size("tp"), rows_dev, shared_out.shape[-1])
    terms_out = pieces.astype(jnp.bfloat16)
    summed = (
        lax.psum_scatter(
            lax.optimization_barrier(terms_out).astype(jnp.float32).astype(jnp.bfloat16),
            "tp",
            scatter_dimension=0,
            tiled=True,
        )
        .astype(jnp.float32)[0]
        .astype(jnp.bfloat16)
    )
    returned = lax.all_to_all(local_routed, "sp", split_axis=0, concat_axis=0, tiled=True)
    picked = (
        returned[targets].reshape(rows_dev, route_count, returned.shape[-1]).astype(jnp.float32)
    )
    routed_sum = jnp.sum(route_weight[:, :, None] * picked, axis=1)
    return (stream_wide + summed.astype(jnp.float32) + routed_sum).astype(jnp.bfloat16)


MESH = pl.DeviceIdType.MESH


def peer_barrier(peers):
    barrier = pltpu.get_barrier_semaphore()
    for peer in peers:
        pl.semaphore_signal(barrier, inc=1, device_id=peer, device_id_type=MESH)
    pl.semaphore_wait(barrier, len(peers))


def remote(src, dst, send_sem, recv_sem, peer):
    return pltpu.make_async_remote_copy(
        src_ref=src,
        dst_ref=dst,
        send_sem=send_sem,
        recv_sem=recv_sem,
        device_id=peer,
        device_id_type=MESH,
    )


def grid_place(sp):
    s = lax.axis_index("sp")
    t = lax.axis_index("tp")
    return s, t, s // 2, s % 2, sp // 2


def gather_kernel(sp, tp, count, with_tp, *refs):
    ins, refs = refs[:count], refs[count:]
    outs, refs = refs[:count], refs[count:]
    if with_tp:
        tp_out, refs = refs[0], refs[1:]
    send_sem, recv_sem, local_sem = refs[:3]
    s, t, z, x, depth = grid_place(sp)
    line = [(lax.rem(z + k, depth) * 2 + x, t) for k in range(1, depth)]
    across = (z * 2 + (1 - x), t)
    columns = [(s, lax.rem(t + k, tp)) for k in range(1, tp)] if with_tp else []
    peer_barrier(line + [across] + columns)
    copies = []
    arrivals = []
    for i in range(count):
        for k in range(depth - 1, 0, -1):
            copy = remote(
                ins[i], outs[i].at[s], send_sem.at[i, k], recv_sem.at[i, k], line[k - 1]
            )
            copy.start()
            copies.append(copy)
            arrivals.append((k, i, copy))
    for i in range(count):
        copy = remote(
            ins[i], outs[i].at[s], send_sem.at[i, depth], recv_sem.at[i, depth], across
        )
        copy.start()
        copies.append(copy)
    side = []
    if with_tp:
        for k in range(1, tp):
            copy = remote(
                ins[0],
                tp_out.at[t],
                send_sem.at[0, 2 * depth + k],
                recv_sem.at[0, 2 * depth + k],
                columns[k - 1],
            )
            copy.start()
            side.append(copy)
        own = pltpu.make_async_copy(ins[0], tp_out.at[t], local_sem.at[count])
        own.start()
    locals_ = []
    for i in range(count):
        copy = pltpu.make_async_copy(ins[i], outs[i].at[s], local_sem.at[i])
        copy.start()
        locals_.append(copy)
    order = {1: 0, 3: 1, 2: 2}
    arrivals.sort(key=lambda item: (order.get(item[0], item[0]), item[1]))
    for k, i, copy in arrivals:
        copy.wait_recv()
        origin = lax.rem(z + depth - k, depth) * 2 + x
        relay = remote(
            outs[i].at[origin],
            outs[i].at[origin],
            send_sem.at[i, depth + k],
            recv_sem.at[i, depth + k],
            across,
        )
        relay.start()
        side.append(relay)
    for _, _, copy in arrivals:
        copy.wait_send()
    for copy in copies:
        if not any(copy is entry[2] for entry in arrivals):
            copy.wait()
    for copy in side:
        copy.wait()
    for copy in locals_:
        copy.wait()
    if with_tp:
        own.wait()


def gather_sp(arrays, sp, tp, with_tp, collective_id):
    count = len(arrays)
    depth = sp // 2
    shapes = [jax.ShapeDtypeStruct((sp,) + a.shape, a.dtype) for a in arrays]
    if with_tp:
        shapes.append(jax.ShapeDtypeStruct((tp,) + arrays[0].shape, arrays[0].dtype))
    slots = 2 * depth + tp
    return pl.pallas_call(
        partial(gather_kernel, sp, tp, count, with_tp),
        out_shape=tuple(shapes),
        in_specs=[pl.BlockSpec(memory_space=pltpu.VMEM)] * count,
        out_specs=tuple([pl.BlockSpec(memory_space=pltpu.VMEM)] * len(shapes)),
        scratch_shapes=[
            pltpu.SemaphoreType.DMA((count, slots)),
            pltpu.SemaphoreType.DMA((count, slots)),
            pltpu.SemaphoreType.DMA((count + 1,)),
        ],
        compiler_params=pltpu.CompilerParams(
            collective_id=collective_id, has_side_effects=True
        ),
        cost_estimate=pl.CostEstimate(flops=0, bytes_accessed=40_000_000, transcendentals=0),
    )(*arrays)


def heads_kernel(tp, x_ref, out_ref, send_sem, recv_sem, local_sem):
    s = lax.axis_index("sp")
    t = lax.axis_index("tp")
    width = x_ref.shape[1]
    peers = [(s, lax.rem(t + k, tp)) for k in range(1, tp)]
    peer_barrier(peers)
    mine = pl.ds(pl.multiple_of(t * width, width), width)
    copies = []
    for k in range(1, tp):
        copy = remote(
            x_ref, out_ref.at[:, mine], send_sem.at[k], recv_sem.at[k], peers[k - 1]
        )
        copy.start()
        copies.append(copy)
    own = pltpu.make_async_copy(x_ref, out_ref.at[:, mine], local_sem)
    own.start()
    for copy in copies:
        copy.wait()
    own.wait()


def gather_heads(attended, tp, collective_id):
    tokens, width = attended.shape
    return pl.pallas_call(
        partial(heads_kernel, tp),
        out_shape=jax.ShapeDtypeStruct((tokens, tp * width), attended.dtype),
        in_specs=[pl.BlockSpec(memory_space=pltpu.VMEM)],
        out_specs=pl.BlockSpec(memory_space=pltpu.VMEM),
        scratch_shapes=[
            pltpu.SemaphoreType.DMA((tp,)),
            pltpu.SemaphoreType.DMA((tp,)),
            pltpu.SemaphoreType.DMA,
        ],
        compiler_params=pltpu.CompilerParams(
            collective_id=collective_id, has_side_effects=True
        ),
        cost_estimate=pl.CostEstimate(flops=0, bytes_accessed=20_000_000, transcendentals=0),
    )(attended)


def return_kernel(
    sp,
    tp,
    routed_ref,
    shared_ref,
    stream_ref,
    out_ref,
    from_across,
    pair_sum,
    from_line,
    from_column,
    send_sem,
    recv_sem,
):
    s, t, z, x, depth = grid_place(sp)
    line = [(lax.rem(z + k, depth) * 2 + x, t) for k in range(1, depth)]
    across = (z * 2 + (1 - x), t)
    columns = [(s, lax.rem(t + k, tp)) for k in range(1, tp)]
    peer_barrier(line + [across] + columns)
    order = [2, 3, 1] if depth == 4 else list(range(1, depth))
    crossing = {}
    for k in order + [0]:
        target = lax.rem(z + k, depth) * 2 + (1 - x)
        copy = remote(
            routed_ref.at[target], from_across.at[k], send_sem.at[k], recv_sem.at[k], across
        )
        copy.start()
        crossing[k] = copy
    side = []
    for k in range(1, tp):
        copy = remote(
            shared_ref.at[lax.rem(t + k, tp)],
            from_column.at[k - 1],
            send_sem.at[2 * depth + k],
            recv_sem.at[2 * depth + k],
            columns[k - 1],
        )
        copy.start()
        side.append(copy)
    moving = []
    for k in order:
        crossing[k].wait_recv()
        target = lax.rem(z + k, depth) * 2 + x
        pair_sum[k - 1] = (
            routed_ref[target].astype(jnp.float32) + from_across[k].astype(jnp.float32)
        ).astype(jnp.bfloat16)
        copy = remote(
            pair_sum.at[k - 1],
            from_line.at[k - 1],
            send_sem.at[depth + k],
            recv_sem.at[depth + k],
            line[k - 1],
        )
        copy.start()
        moving.append(copy)
    total = stream_ref[...].astype(jnp.float32) + shared_ref[t].astype(jnp.float32)
    for k, copy in enumerate(side):
        copy.wait_recv()
        total = total + from_column[k].astype(jnp.float32)
    crossing[0].wait_recv()
    total = total + routed_ref[s].astype(jnp.float32) + from_across[0].astype(jnp.float32)
    for k, copy in zip(order, moving):
        copy.wait_recv()
        total = total + from_line[k - 1].astype(jnp.float32)
    out_ref[...] = total.astype(out_ref.dtype)
    for copy in list(crossing.values()) + side + moving:
        copy.wait_send()


def return_rows(routed, shared, stream, sp, tp, collective_id):
    rows, width = stream.shape
    depth = sp // 2
    slots = 2 * depth + tp
    return pl.pallas_call(
        partial(return_kernel, sp, tp),
        out_shape=jax.ShapeDtypeStruct((rows, width), jnp.bfloat16),
        in_specs=[pl.BlockSpec(memory_space=pltpu.VMEM)] * 3,
        out_specs=pl.BlockSpec(memory_space=pltpu.VMEM),
        scratch_shapes=[
            pltpu.VMEM((depth, rows, width), jnp.bfloat16),
            pltpu.VMEM((depth - 1, rows, width), jnp.bfloat16),
            pltpu.VMEM((depth - 1, rows, width), jnp.bfloat16),
            pltpu.VMEM((tp - 1, rows, width), jnp.bfloat16),
            pltpu.SemaphoreType.DMA((slots,)),
            pltpu.SemaphoreType.DMA((slots,)),
        ],
        compiler_params=pltpu.CompilerParams(
            collective_id=collective_id, has_side_effects=True
        ),
        cost_estimate=pl.CostEstimate(flops=0, bytes_accessed=60_000_000, transcendentals=0),
    )(routed, shared, stream)


def experts_kernel(groups, *refs):
    rows_ref, weight_ref = refs[:2]
    parts = [refs[2 + 4 * q : 6 + 4 * q] for q in range(groups)]
    out_ref, gate_buf, up_buf, down_buf, total, sems = refs[2 + 4 * groups :]
    copies = []
    for q in range(groups):
        half = parts[q][2].shape[0]
        places = (
            gate_buf.at[q],
            up_buf.at[q],
            down_buf.at[q, pl.ds(0, half)],
            down_buf.at[q, pl.ds(half, half)],
        )
        for n, (source, place) in enumerate(zip(parts[q], places)):
            copy = pltpu.make_async_copy(source, place, sems.at[q, n])
            copy.start()
            copies.append(copy)
    for q in range(groups):
        copies[4 * q].wait()
        gate_value = jnp.dot(rows_ref[...], gate_buf[q], preferred_element_type=jnp.float32)
        copies[4 * q + 1].wait()
        up_value = jnp.dot(rows_ref[...], up_buf[q], preferred_element_type=jnp.float32)
        hidden = (jax.nn.silu(gate_value) * up_value).astype(jnp.bfloat16)
        copies[4 * q + 2].wait()
        copies[4 * q + 3].wait()
        product = jnp.dot(hidden, down_buf[q], preferred_element_type=jnp.float32)
        if q == 0:
            total[...] = product
        elif q < groups - 1:
            total[...] += product
        else:
            out_ref[...] = ((total[...] + product) * weight_ref[...]).astype(jnp.bfloat16)


def run_experts(rows_in, dense_weight, parts):
    groups = len(parts)
    count, width = rows_in.shape
    units = parts[0][0].shape[1]
    flat = [array for part in parts for array in part]
    return pl.pallas_call(
        partial(experts_kernel, groups),
        out_shape=jax.ShapeDtypeStruct((count, width), jnp.bfloat16),
        in_specs=[pl.BlockSpec(memory_space=pltpu.VMEM)] * 2
        + [pl.BlockSpec(memory_space=pl.ANY)] * len(flat),
        out_specs=pl.BlockSpec(memory_space=pltpu.VMEM),
        scratch_shapes=[
            pltpu.VMEM((groups, width, units), jnp.bfloat16),
            pltpu.VMEM((groups, width, units), jnp.bfloat16),
            pltpu.VMEM((groups, units, width), jnp.bfloat16),
            pltpu.VMEM((count, width), jnp.float32),
            pltpu.SemaphoreType.DMA((groups, 4)),
        ],
        compiler_params=pltpu.CompilerParams(vmem_limit_bytes=40 * 1024 * 1024),
        cost_estimate=pl.CostEstimate(
            flops=6 * count * width * units * groups,
            bytes_accessed=12_000_000,
            transcendentals=0,
        ),
    )(rows_in, dense_weight, *flat)


def dense_body(
    query_maps,
    key_maps,
    value_rows,
    mix_lambda,
    head_gain,
    out_weight,
    residual,
    norm_gain,
    routes,
    route_weight,
    expert_gate,
    expert_up,
    expert_down,
    shared_gate,
    shared_up,
    shared_down,
):
    sp = lax.axis_size("sp")
    tp = lax.axis_size("tp")
    s = lax.axis_index("sp")
    t = lax.axis_index("tp")

    def swapped(array, step):
        return lax.ppermute(array, "tp", [(i, i ^ step) for i in range(tp)])

    half = expert_down.shape[1] // 2
    own_gate, own_up = expert_gate[0], expert_up[0]
    own_low, own_high = expert_down[0, :half], expert_down[0, half:]
    far_residual = swapped(residual, 2)
    far_gate = swapped(own_gate, 2)
    far_low = swapped(own_low, 2)
    near_residual = swapped(residual, 1)
    near_gate, near_up, near_low, near_high = (
        swapped(a, 1) for a in (own_gate, own_up, own_low, own_high)
    )
    odd, upper = t % 2 == 1, t // 2 == 1

    def in_order(first, second, turned):
        return jnp.where(
            turned,
            jnp.concatenate([second, first], axis=0),
            jnp.concatenate([first, second], axis=0),
        )

    column_residual = in_order(
        in_order(residual, near_residual, odd),
        in_order(far_residual, swapped(far_residual, 1), odd),
        upper,
    )

    local_heads = mix_lambda.shape[0]
    head_width = head_gain.shape[0]
    kv_local = value_rows.shape[1] // head_width
    head_group = local_heads // kv_local
    head_dim = key_maps.shape[1] // (2 * kv_local)
    token_count = query_maps.shape[0]
    rows_dev = token_count // tp
    experts = sp

    own_routes = lax.dynamic_slice_in_dim(routes, t * rows_dev, rows_dev, 0)
    named = own_routes[None, :, :] == jnp.arange(experts, dtype=jnp.int32)[:, None, None]
    table = jnp.sum(jnp.where(named, route_weight[None], 0.0), axis=2)
    lanes = -(-rows_dev // 128) * 128
    table = jnp.pad(table, ((0, 0), (0, lanes - rows_dev)))

    key_all, value_all = gather_sp([key_maps, value_rows], sp, tp, False, 1)
    key_all = key_all.reshape(sp * token_count, -1)
    value_all = value_all.reshape(sp * token_count, -1)

    queries = query_maps.reshape(token_count, kv_local, head_group, 2, head_dim)
    start_max = jnp.full((kv_local, head_group, 2, token_count), lowest_score, jnp.float32)
    start_sum = jnp.zeros((kv_local, head_group, 2, token_count), jnp.float32)
    start_values = jnp.zeros((kv_local, head_group, 2, token_count, head_width), jnp.float32)
    _, run_sum, accumulated = fold_keys(
        (start_max, start_sum, start_values),
        (key_all, value_all),
        jnp.int32(0),
        queries,
        head_dim ** (-0.5),
    )
    normalized = accumulated / run_sum[..., None]
    lambdas = mix_lambda.reshape(kv_local, head_group, 1, 1)
    difference = normalized[:, :, 0] - lambdas * normalized[:, :, 1]
    inverse_rms = lax.rsqrt(jnp.mean(difference * difference, axis=-1, keepdims=True) + norm_eps)
    head_scaled = (difference * inverse_rms * head_gain).astype(jnp.bfloat16)
    attended = jnp.transpose(head_scaled, (2, 0, 1, 3)).reshape(
        token_count, local_heads * head_width
    )
    attended = gather_heads(attended, tp, 2)
    attended, late_up, late_high = lax.optimization_barrier((attended, own_up, own_high))
    far_up = swapped(late_up, 2)
    far_high = swapped(late_high, 2)
    projected = jnp.dot(attended, out_weight, preferred_element_type=jnp.float32)
    streams = (column_residual.astype(jnp.float32) + projected).astype(jnp.bfloat16)
    stream_wide = streams.astype(jnp.float32)
    stream_rms = lax.rsqrt(jnp.mean(stream_wide * stream_wide, axis=1, keepdims=True) + norm_eps)
    shared_in = (stream_wide * stream_rms * norm_gain).astype(jnp.bfloat16)
    stream = lax.dynamic_slice_in_dim(streams, t * rows_dev, rows_dev, 0)
    normed = lax.dynamic_slice_in_dim(shared_in, t * rows_dev, rows_dev, 0)

    routed_in, tables = gather_sp([normed, table], sp, tp, False, 3)
    dense_weight = lax.dynamic_index_in_dim(tables, s, 1, False)[:, :rows_dev]
    dense_weight = dense_weight.reshape(sp * rows_dev, 1)
    width = normed.shape[1]
    shared_hidden = (
        jax.nn.silu(jnp.dot(shared_in, shared_gate, preferred_element_type=jnp.float32))
        * jnp.dot(shared_in, shared_up, preferred_element_type=jnp.float32)
    ).astype(jnp.bfloat16)
    shared_out = jnp.dot(shared_hidden, shared_down, preferred_element_type=jnp.float32)
    shared_out = shared_out.astype(jnp.bfloat16).reshape(tp, rows_dev, width)

    near_far = tuple(swapped(a, 1) for a in (far_gate, far_up, far_low, far_high))
    routed = run_experts(
        routed_in.reshape(sp * rows_dev, width),
        dense_weight,
        (
            (own_gate, own_up, own_low, own_high),
            (near_gate, near_up, near_low, near_high),
            (far_gate, far_up, far_low, far_high),
            near_far,
        ),
    )
    return return_rows(routed.reshape(sp, rows_dev, width), shared_out, stream, sp, tp, 4)


def solution(mesh):
    in_specs = (
        P("sp", "tp"),
        P("sp", "tp"),
        P("sp", "tp"),
        P("tp"),
        P(),
        P(),
        P(("sp", "tp"), None),
        P(),
        P("sp", None),
        P(("sp", "tp"), None),
        P("sp", None, "tp"),
        P("sp", None, "tp"),
        P("sp", "tp", None),
        P(None, "tp"),
        P(None, "tp"),
        P("tp", None),
    )
    out_specs = P(("sp", "tp"), None)
    sp, tp = mesh.shape["sp"], mesh.shape["tp"]

    def chosen(*args):
        route_count = args[8].shape[1]
        experts = sp * args[10].shape[0]
        rows_dev = args[6].shape[0]
        whole_blocks = 2 * rows_dev * route_count >= experts * rows_dev
        dense = whole_blocks and args[10].shape[0] == 1 and sp == 8 and tp == 4
        if not dense:
            return body(*args)
        return dense_body(*args)

    return jax.shard_map(
        chosen, mesh=mesh, in_specs=in_specs, out_specs=out_specs, check_vma=False
    )
```

```python
from functools import partial

import jax
import jax.numpy as jnp
from jax import lax
from jax.experimental import pallas as pl
from jax.experimental.pallas import tpu as pltpu
from jax.sharding import PartitionSpec as P


norm_eps = 1e-06
lowest_score = -1e30


def slot_targets(block_routes, experts, capacity):
    flat_routes = block_routes.reshape(-1)
    onehot = (flat_routes[:, None] == jnp.arange(experts, dtype=jnp.int32)[None, :]).astype(
        jnp.int32
    )
    earlier = jnp.cumsum(onehot, axis=0) - onehot
    return flat_routes * capacity + jnp.sum(earlier * onehot, axis=1)


def build_buffer(token_rows, block_routes, experts, capacity):
    targets = slot_targets(block_routes, experts, capacity)
    row_total = block_routes.shape[0]
    route_count = block_routes.shape[1]
    source_row = jnp.arange(row_total * route_count, dtype=jnp.int32) // route_count
    holder = jnp.full((experts * capacity,), row_total, jnp.int32).at[targets].set(source_row)
    padded = jnp.concatenate(
        [token_rows, jnp.zeros((1, token_rows.shape[1]), token_rows.dtype)], axis=0
    )
    return (padded[holder], targets)


def attention_block(carried, queries, key_block, value_block, score_scale):
    run_max, run_sum, accumulated = carried
    kv_local = run_max.shape[0]
    key_heads = key_block.reshape(key_block.shape[0], kv_local, 2, -1)
    value_heads = value_block.reshape(value_block.shape[0], kv_local, -1)
    scores = (
        jnp.einsum("qagcd,racd->agcqr", queries, key_heads, preferred_element_type=jnp.float32)
        * score_scale
    )
    new_max = jnp.maximum(run_max, jnp.max(scores, axis=-1))
    rescale = jnp.exp(run_max - new_max)
    weights = jnp.exp(scores - new_max[..., None])
    run_sum = run_sum * rescale + jnp.sum(weights, axis=-1)
    update = jnp.einsum(
        "agcqr,rae->agcqe",
        weights.astype(jnp.bfloat16),
        value_heads,
        preferred_element_type=jnp.float32,
    )
    return (new_max, run_sum, accumulated * rescale[..., None] + update)


def fold_keys(carried, pieces, first_row, queries, score_scale):
    key_piece, value_piece = pieces
    total_rows = key_piece.shape[0]
    block_rows = total_rows
    for candidate in (2048, 1024, 512):
        if total_rows % candidate == 0:
            block_rows = candidate
            break
    block_count = total_rows // block_rows

    def block_step(block_index, running):
        start_row = block_index * block_rows
        return attention_block(
            running,
            queries,
            lax.dynamic_slice_in_dim(key_piece, start_row, block_rows, 0),
            lax.dynamic_slice_in_dim(value_piece, start_row, block_rows, 0),
            score_scale,
        )

    return lax.fori_loop(0, block_count, block_step, carried)


def whole_experts(arrived, whole_gate, whole_up, whole_down, senders, capacity, groups):
    local_experts = whole_gate.shape[0]
    width = arrived.shape[-1]
    rows_in = arrived.reshape(senders, local_experts, capacity, width)
    gate_value = jnp.einsum(
        "sjtd,jdf->sjtf", rows_in, whole_gate, preferred_element_type=jnp.float32
    )
    up_value = jnp.einsum("sjtd,jdf->sjtf", rows_in, whole_up, preferred_element_type=jnp.float32)
    hidden = (jax.nn.silu(gate_value) * up_value).astype(jnp.bfloat16)
    hidden_units = hidden.shape[-1]
    hidden = hidden.reshape(senders, local_experts, capacity, groups, hidden_units // groups)
    down_groups = whole_down.reshape(local_experts, groups, hidden_units // groups, width)
    group_sums = jnp.einsum(
        "sjtgf,jgfd->sjtgd", hidden, down_groups, preferred_element_type=jnp.float32
    )
    group_sums = lax.optimization_barrier(group_sums.astype(jnp.bfloat16)).astype(jnp.float32)
    return (
        jnp.sum(group_sums, axis=3)
        .astype(jnp.bfloat16)
        .reshape(senders * local_experts * capacity, width)
    )


def body(
    query_maps,
    key_maps,
    value_rows,
    mix_lambda,
    head_gain,
    out_weight,
    residual,
    norm_gain,
    routes,
    route_weight,
    expert_gate,
    expert_up,
    expert_down,
    shared_gate,
    shared_up,
    shared_down,
):
    local_heads = mix_lambda.shape[0]
    head_width = head_gain.shape[0]
    kv_local = value_rows.shape[1] // head_width
    head_group = local_heads // kv_local
    head_dim = key_maps.shape[1] // (2 * kv_local)
    token_count = query_maps.shape[0]
    queries = query_maps.reshape(token_count, kv_local, head_group, 2, head_dim)
    start_max = jnp.full((kv_local, head_group, 2, token_count), lowest_score, jnp.float32)
    start_sum = jnp.zeros((kv_local, head_group, 2, token_count), jnp.float32)
    start_values = jnp.zeros((kv_local, head_group, 2, token_count, head_width), jnp.float32)
    folder = partial(fold_keys, queries=queries, score_scale=head_dim ** (-0.5))
    _, run_sum, accumulated = folder(
        (start_max, start_sum, start_values),
        (
            lax.all_gather(key_maps, "sp", axis=0, tiled=True),
            lax.all_gather(value_rows, "sp", axis=0, tiled=True),
        ),
        jnp.int32(0),
    )
    normalized = accumulated / run_sum[..., None]
    lambdas = mix_lambda.reshape(kv_local, head_group, 1, 1)
    difference = normalized[:, :, 0] - lambdas * normalized[:, :, 1]
    inverse_rms = lax.rsqrt(jnp.mean(difference * difference, axis=-1, keepdims=True) + norm_eps)
    head_scaled = (difference * inverse_rms * head_gain).astype(jnp.bfloat16)
    attended = jnp.transpose(head_scaled, (2, 0, 1, 3)).reshape(
        token_count, local_heads * head_width
    )
    columns = lax.axis_size("tp")
    column = lax.axis_index("tp")
    rows_dev = token_count // columns
    own_rows = lax.dynamic_slice_in_dim(
        out_weight, column * attended.shape[1], attended.shape[1], 0
    )
    projected = lax.psum_scatter(
        jnp.dot(attended, own_rows, preferred_element_type=jnp.float32).astype(jnp.bfloat16),
        "tp",
        scatter_dimension=0,
        tiled=True,
    ).astype(jnp.float32)
    stream = (residual.astype(jnp.float32) + projected).astype(jnp.bfloat16)
    stream_wide = stream.astype(jnp.float32)
    stream_rms = lax.rsqrt(jnp.mean(stream_wide * stream_wide, axis=1, keepdims=True) + norm_eps)
    normed = (stream_wide * stream_rms * norm_gain).astype(jnp.bfloat16)
    senders = lax.axis_size("sp")
    local_experts = expert_gate.shape[0]
    experts = senders * local_experts
    route_count = routes.shape[1]
    capacity = max(2, 2 * rows_dev * route_count // experts)
    local_routed = None
    whole_gate, whole_up, whole_down = (
        lax.all_gather(expert_gate, "tp", axis=2, tiled=True),
        lax.all_gather(expert_up, "tp", axis=2, tiled=True),
        lax.all_gather(expert_down, "tp", axis=1, tiled=True),
    )
    own_routes = lax.dynamic_slice_in_dim(routes, column * rows_dev, rows_dev, 0)
    buffer, targets = build_buffer(normed, own_routes, experts, capacity)
    arrived = lax.all_to_all(buffer, "sp", split_axis=0, concat_axis=0, tiled=True)
    local_routed = whole_experts(
        arrived, whole_gate, whole_up, whole_down, senders, capacity, columns
    )
    shared_rows = lax.all_gather(normed[None], "tp", axis=0, tiled=True)
    shared_in = shared_rows
    shared_in = shared_in.reshape(1 * lax.axis_size("tp") * rows_dev, shared_in.shape[-1])
    shared_hidden = (
        jax.nn.silu(jnp.dot(shared_in, shared_gate, preferred_element_type=jnp.float32))
        * jnp.dot(shared_in, shared_up, preferred_element_type=jnp.float32)
    ).astype(jnp.bfloat16)
    shared_out = jnp.dot(shared_hidden, shared_down, preferred_element_type=jnp.float32)
    pieces = shared_out.reshape(1 * lax.axis_size("tp"), rows_dev, shared_out.shape[-1])
    terms_out = pieces.astype(jnp.bfloat16)
    summed = (
        lax.psum_scatter(
            lax.optimization_barrier(terms_out).astype(jnp.float32).astype(jnp.bfloat16),
            "tp",
            scatter_dimension=0,
            tiled=True,
        )
        .astype(jnp.float32)[0]
        .astype(jnp.bfloat16)
    )
    returned = lax.all_to_all(local_routed, "sp", split_axis=0, concat_axis=0, tiled=True)
    picked = (
        returned[targets].reshape(rows_dev, route_count, returned.shape[-1]).astype(jnp.float32)
    )
    routed_sum = jnp.sum(route_weight[:, :, None] * picked, axis=1)
    return (stream_wide + summed.astype(jnp.float32) + routed_sum).astype(jnp.bfloat16)


MESH = pl.DeviceIdType.MESH


def peer_barrier(peers):
    barrier = pltpu.get_barrier_semaphore()
    for peer in peers:
        pl.semaphore_signal(barrier, inc=1, device_id=peer, device_id_type=MESH)
    pl.semaphore_wait(barrier, len(peers))


def remote(src, dst, send_sem, recv_sem, peer):
    return pltpu.make_async_remote_copy(
        src_ref=src,
        dst_ref=dst,
        send_sem=send_sem,
        recv_sem=recv_sem,
        device_id=peer,
        device_id_type=MESH,
    )


def grid_place(sp):
    s = lax.axis_index("sp")
    t = lax.axis_index("tp")
    return s, t, s // 2, s % 2, sp // 2


def gather_kernel(sp, tp, count, with_tp, *refs):
    ins, refs = refs[:count], refs[count:]
    outs, refs = refs[:count], refs[count:]
    if with_tp:
        tp_out, refs = refs[0], refs[1:]
    send_sem, recv_sem, local_sem = refs[:3]
    s, t, z, x, depth = grid_place(sp)
    line = [(lax.rem(z + k, depth) * 2 + x, t) for k in range(1, depth)]
    across = (z * 2 + (1 - x), t)
    columns = [(s, lax.rem(t + k, tp)) for k in range(1, tp)] if with_tp else []
    peer_barrier(line + [across] + columns)
    copies = []
    arrivals = []
    for i in range(count):
        for k in (1, 3, 2) if depth == 4 else range(1, depth):
            copy = remote(
                ins[i], outs[i].at[s], send_sem.at[i, k], recv_sem.at[i, k], line[k - 1]
            )
            copy.start()
            copies.append(copy)
            arrivals.append((k, i, copy))
    for i in range(count):
        copy = remote(
            ins[i], outs[i].at[s], send_sem.at[i, depth], recv_sem.at[i, depth], across
        )
        copy.start()
        copies.append(copy)
    side = []
    if with_tp:
        for k in range(1, tp):
            copy = remote(
                ins[0],
                tp_out.at[t],
                send_sem.at[0, 2 * depth + k],
                recv_sem.at[0, 2 * depth + k],
                columns[k - 1],
            )
            copy.start()
            side.append(copy)
        own = pltpu.make_async_copy(ins[0], tp_out.at[t], local_sem.at[count])
        own.start()
    locals_ = []
    for i in range(count):
        copy = pltpu.make_async_copy(ins[i], outs[i].at[s], local_sem.at[i])
        copy.start()
        locals_.append(copy)
    order = {1: 0, 3: 1, 2: 2}
    arrivals.sort(key=lambda item: (order.get(item[0], item[0]), item[1]))
    for k, i, copy in arrivals:
        copy.wait_recv()
        origin = lax.rem(z + depth - k, depth) * 2 + x
        relay = remote(
            outs[i].at[origin],
            outs[i].at[origin],
            send_sem.at[i, depth + k],
            recv_sem.at[i, depth + k],
            across,
        )
        relay.start()
        side.append(relay)
    for _, _, copy in arrivals:
        copy.wait_send()
    for copy in copies:
        if not any(copy is entry[2] for entry in arrivals):
            copy.wait()
    for copy in side:
        copy.wait()
    for copy in locals_:
        copy.wait()
    if with_tp:
        own.wait()


def gather_sp(arrays, sp, tp, with_tp, collective_id):
    count = len(arrays)
    depth = sp // 2
    shapes = [jax.ShapeDtypeStruct((sp,) + a.shape, a.dtype) for a in arrays]
    if with_tp:
        shapes.append(jax.ShapeDtypeStruct((tp,) + arrays[0].shape, arrays[0].dtype))
    slots = 2 * depth + tp
    return pl.pallas_call(
        partial(gather_kernel, sp, tp, count, with_tp),
        out_shape=tuple(shapes),
        in_specs=[pl.BlockSpec(memory_space=pltpu.VMEM)] * count,
        out_specs=tuple([pl.BlockSpec(memory_space=pltpu.VMEM)] * len(shapes)),
        scratch_shapes=[
            pltpu.SemaphoreType.DMA((count, slots)),
            pltpu.SemaphoreType.DMA((count, slots)),
            pltpu.SemaphoreType.DMA((count + 1,)),
        ],
        compiler_params=pltpu.CompilerParams(
            collective_id=collective_id,
            has_side_effects=True,
            vmem_limit_bytes=16 * 1024 * 1024,
        ),
        cost_estimate=pl.CostEstimate(flops=0, bytes_accessed=40_000_000, transcendentals=0),
    )(*arrays)


def heads_kernel(tp, x_ref, out_ref, send_sem, recv_sem, local_sem):
    s = lax.axis_index("sp")
    t = lax.axis_index("tp")
    width = x_ref.shape[1]
    peers = [(s, lax.rem(t + k, tp)) for k in range(1, tp)]
    peer_barrier(peers)
    mine = pl.ds(pl.multiple_of(t * width, width), width)
    copies = []
    for k in range(1, tp):
        copy = remote(
            x_ref, out_ref.at[:, mine], send_sem.at[k], recv_sem.at[k], peers[k - 1]
        )
        copy.start()
        copies.append(copy)
    own = pltpu.make_async_copy(x_ref, out_ref.at[:, mine], local_sem)
    own.start()
    for copy in copies:
        copy.wait()
    own.wait()


def gather_heads(attended, tp, collective_id):
    tokens, width = attended.shape
    return pl.pallas_call(
        partial(heads_kernel, tp),
        out_shape=jax.ShapeDtypeStruct((tokens, tp * width), attended.dtype),
        in_specs=[pl.BlockSpec(memory_space=pltpu.VMEM)],
        out_specs=pl.BlockSpec(memory_space=pltpu.VMEM),
        scratch_shapes=[
            pltpu.SemaphoreType.DMA((tp,)),
            pltpu.SemaphoreType.DMA((tp,)),
            pltpu.SemaphoreType.DMA,
        ],
        compiler_params=pltpu.CompilerParams(
            collective_id=collective_id,
            has_side_effects=True,
            vmem_limit_bytes=16 * 1024 * 1024,
        ),
        cost_estimate=pl.CostEstimate(flops=0, bytes_accessed=20_000_000, transcendentals=0),
    )(attended)


def return_kernel(
    sp,
    tp,
    routed_ref,
    shared_ref,
    stream_ref,
    out_ref,
    from_across,
    pair_sum,
    from_line,
    from_column,
    send_sem,
    recv_sem,
):
    s, t, z, x, depth = grid_place(sp)
    line = [(lax.rem(z + k, depth) * 2 + x, t) for k in range(1, depth)]
    across = (z * 2 + (1 - x), t)
    columns = [(s, lax.rem(t + k, tp)) for k in range(1, tp)]
    peer_barrier(line + [across] + columns)
    order = [2, 3, 1] if depth == 4 else list(range(1, depth))
    crossing = {}
    for k in order + [0]:
        target = lax.rem(z + k, depth) * 2 + (1 - x)
        copy = remote(
            routed_ref.at[target], from_across.at[k], send_sem.at[k], recv_sem.at[k], across
        )
        copy.start()
        crossing[k] = copy
    side = []
    for k in range(1, tp):
        copy = remote(
            shared_ref.at[lax.rem(t + k, tp)],
            from_column.at[k - 1],
            send_sem.at[2 * depth + k],
            recv_sem.at[2 * depth + k],
            columns[k - 1],
        )
        copy.start()
        side.append(copy)
    moving = []
    for k in order:
        crossing[k].wait_recv()
        target = lax.rem(z + k, depth) * 2 + x
        pair_sum[k - 1] = (
            routed_ref[target].astype(jnp.float32) + from_across[k].astype(jnp.float32)
        ).astype(jnp.bfloat16)
        copy = remote(
            pair_sum.at[k - 1],
            from_line.at[k - 1],
            send_sem.at[depth + k],
            recv_sem.at[depth + k],
            line[k - 1],
        )
        copy.start()
        moving.append(copy)
    total = stream_ref[...].astype(jnp.float32) + shared_ref[t].astype(jnp.float32)
    for k, copy in enumerate(side):
        copy.wait_recv()
        total = total + from_column[k].astype(jnp.float32)
    crossing[0].wait_recv()
    total = total + routed_ref[s].astype(jnp.float32) + from_across[0].astype(jnp.float32)
    for k, copy in zip(order, moving):
        copy.wait_recv()
        total = total + from_line[k - 1].astype(jnp.float32)
    out_ref[...] = total.astype(out_ref.dtype)
    for copy in list(crossing.values()) + side + moving:
        copy.wait_send()


def return_rows(routed, shared, stream, sp, tp, collective_id):
    rows, width = stream.shape
    depth = sp // 2
    slots = 2 * depth + tp
    return pl.pallas_call(
        partial(return_kernel, sp, tp),
        out_shape=jax.ShapeDtypeStruct((rows, width), jnp.bfloat16),
        in_specs=[pl.BlockSpec(memory_space=pltpu.VMEM)] * 3,
        out_specs=pl.BlockSpec(memory_space=pltpu.VMEM),
        scratch_shapes=[
            pltpu.VMEM((depth, rows, width), jnp.bfloat16),
            pltpu.VMEM((depth - 1, rows, width), jnp.bfloat16),
            pltpu.VMEM((depth - 1, rows, width), jnp.bfloat16),
            pltpu.VMEM((tp - 1, rows, width), jnp.bfloat16),
            pltpu.SemaphoreType.DMA((slots,)),
            pltpu.SemaphoreType.DMA((slots,)),
        ],
        compiler_params=pltpu.CompilerParams(
            collective_id=collective_id,
            has_side_effects=True,
            vmem_limit_bytes=16 * 1024 * 1024,
        ),
        cost_estimate=pl.CostEstimate(flops=0, bytes_accessed=60_000_000, transcendentals=0),
    )(routed, shared, stream)


def experts_kernel(groups, *refs):
    rows_ref, weight_ref = refs[:2]
    parts = [refs[2 + 4 * q : 6 + 4 * q] for q in range(groups)]
    out_ref, gate_buf, up_buf, down_buf, total, sems = refs[2 + 4 * groups :]
    copies = []
    for q in range(groups):
        half = parts[q][2].shape[0]
        places = (
            gate_buf.at[q],
            up_buf.at[q],
            down_buf.at[q, pl.ds(0, half)],
            down_buf.at[q, pl.ds(half, half)],
        )
        for n, (source, place) in enumerate(zip(parts[q], places)):
            copy = pltpu.make_async_copy(source, place, sems.at[q, n])
            copy.start()
            copies.append(copy)
    for q in range(groups):
        copies[4 * q].wait()
        gate_value = jnp.dot(rows_ref[...], gate_buf[q], preferred_element_type=jnp.float32)
        copies[4 * q + 1].wait()
        up_value = jnp.dot(rows_ref[...], up_buf[q], preferred_element_type=jnp.float32)
        hidden = (jax.nn.silu(gate_value) * up_value).astype(jnp.bfloat16)
        copies[4 * q + 2].wait()
        copies[4 * q + 3].wait()
        product = jnp.dot(hidden, down_buf[q], preferred_element_type=jnp.float32)
        if q == 0:
            total[...] = product
        elif q < groups - 1:
            total[...] += product
        else:
            out_ref[...] = ((total[...] + product) * weight_ref[...]).astype(jnp.bfloat16)


def run_experts(rows_in, dense_weight, parts):
    groups = len(parts)
    count, width = rows_in.shape
    units = parts[0][0].shape[1]
    flat = [array for part in parts for array in part]
    return pl.pallas_call(
        partial(experts_kernel, groups),
        out_shape=jax.ShapeDtypeStruct((count, width), jnp.bfloat16),
        in_specs=[pl.BlockSpec(memory_space=pltpu.VMEM)] * 2
        + [pl.BlockSpec(memory_space=pl.ANY)] * len(flat),
        out_specs=pl.BlockSpec(memory_space=pltpu.VMEM),
        scratch_shapes=[
            pltpu.VMEM((groups, width, units), jnp.bfloat16),
            pltpu.VMEM((groups, width, units), jnp.bfloat16),
            pltpu.VMEM((groups, units, width), jnp.bfloat16),
            pltpu.VMEM((count, width), jnp.float32),
            pltpu.SemaphoreType.DMA((groups, 4)),
        ],
        compiler_params=pltpu.CompilerParams(vmem_limit_bytes=40 * 1024 * 1024),
        cost_estimate=pl.CostEstimate(
            flops=6 * count * width * units * groups,
            bytes_accessed=12_000_000,
            transcendentals=0,
        ),
    )(rows_in, dense_weight, *flat)


def dense_body(
    query_maps,
    key_maps,
    value_rows,
    mix_lambda,
    head_gain,
    out_weight,
    residual,
    norm_gain,
    routes,
    route_weight,
    expert_gate,
    expert_up,
    expert_down,
    shared_gate,
    shared_up,
    shared_down,
):
    sp = lax.axis_size("sp")
    tp = lax.axis_size("tp")
    s = lax.axis_index("sp")
    t = lax.axis_index("tp")

    def swapped(array, step):
        return lax.ppermute(array, "tp", [(i, i ^ step) for i in range(tp)])

    half = expert_down.shape[1] // 2
    own_gate, own_up = expert_gate[0], expert_up[0]
    own_low, own_high = expert_down[0, :half], expert_down[0, half:]
    far_residual = swapped(residual, 2)
    far_gate = swapped(own_gate, 2)
    far_low = swapped(own_low, 2)
    near_residual = swapped(residual, 1)
    near_gate, near_up, near_low, near_high = (
        swapped(a, 1) for a in (own_gate, own_up, own_low, own_high)
    )
    odd, upper = t % 2 == 1, t // 2 == 1

    def in_order(first, second, turned):
        return jnp.where(
            turned,
            jnp.concatenate([second, first], axis=0),
            jnp.concatenate([first, second], axis=0),
        )

    column_residual = in_order(
        in_order(residual, near_residual, odd),
        in_order(far_residual, swapped(far_residual, 1), odd),
        upper,
    )

    local_heads = mix_lambda.shape[0]
    head_width = head_gain.shape[0]
    kv_local = value_rows.shape[1] // head_width
    head_group = local_heads // kv_local
    head_dim = key_maps.shape[1] // (2 * kv_local)
    token_count = query_maps.shape[0]
    rows_dev = token_count // tp
    experts = sp

    own_routes = lax.dynamic_slice_in_dim(routes, t * rows_dev, rows_dev, 0)
    named = own_routes[None, :, :] == jnp.arange(experts, dtype=jnp.int32)[:, None, None]
    table = jnp.sum(jnp.where(named, route_weight[None], 0.0), axis=2)
    lanes = -(-rows_dev // 128) * 128
    table = jnp.pad(table, ((0, 0), (0, lanes - rows_dev)))

    key_all, value_all = gather_sp([key_maps, value_rows], sp, tp, False, 1)
    key_all = key_all.reshape(sp * token_count, -1)
    value_all = value_all.reshape(sp * token_count, -1)

    queries = query_maps.reshape(token_count, kv_local, head_group, 2, head_dim)
    start_max = jnp.full((kv_local, head_group, 2, token_count), lowest_score, jnp.float32)
    start_sum = jnp.zeros((kv_local, head_group, 2, token_count), jnp.float32)
    start_values = jnp.zeros((kv_local, head_group, 2, token_count, head_width), jnp.float32)
    _, run_sum, accumulated = fold_keys(
        (start_max, start_sum, start_values),
        (key_all, value_all),
        jnp.int32(0),
        queries,
        head_dim ** (-0.5),
    )
    normalized = accumulated / run_sum[..., None]
    lambdas = mix_lambda.reshape(kv_local, head_group, 1, 1)
    difference = normalized[:, :, 0] - lambdas * normalized[:, :, 1]
    inverse_rms = lax.rsqrt(jnp.mean(difference * difference, axis=-1, keepdims=True) + norm_eps)
    head_scaled = (difference * inverse_rms * head_gain).astype(jnp.bfloat16)
    attended = jnp.transpose(head_scaled, (2, 0, 1, 3)).reshape(
        token_count, local_heads * head_width
    )
    attended = gather_heads(attended, tp, 2)
    attended, late_up, late_high = lax.optimization_barrier((attended, own_up, own_high))
    far_up = swapped(late_up, 2)
    far_high = swapped(late_high, 2)
    projected = jnp.dot(attended, out_weight, preferred_element_type=jnp.float32)
    streams = (column_residual.astype(jnp.float32) + projected).astype(jnp.bfloat16)
    stream_wide = streams.astype(jnp.float32)
    stream_rms = lax.rsqrt(jnp.mean(stream_wide * stream_wide, axis=1, keepdims=True) + norm_eps)
    shared_in = (stream_wide * stream_rms * norm_gain).astype(jnp.bfloat16)
    stream = lax.dynamic_slice_in_dim(streams, t * rows_dev, rows_dev, 0)
    normed = lax.dynamic_slice_in_dim(shared_in, t * rows_dev, rows_dev, 0)

    routed_in, tables = gather_sp([normed, table], sp, tp, False, 3)
    dense_weight = lax.dynamic_index_in_dim(tables, s, 1, False)[:, :rows_dev]
    dense_weight = dense_weight.reshape(sp * rows_dev, 1)
    width = normed.shape[1]
    shared_hidden = (
        jax.nn.silu(jnp.dot(shared_in, shared_gate, preferred_element_type=jnp.float32))
        * jnp.dot(shared_in, shared_up, preferred_element_type=jnp.float32)
    ).astype(jnp.bfloat16)
    shared_out = jnp.dot(shared_hidden, shared_down, preferred_element_type=jnp.float32)
    shared_out = shared_out.astype(jnp.bfloat16).reshape(tp, rows_dev, width)

    near_far = tuple(swapped(a, 1) for a in (far_gate, far_up, far_low, far_high))
    routed = run_experts(
        routed_in.reshape(sp * rows_dev, width),
        dense_weight,
        (
            (own_gate, own_up, own_low, own_high),
            (near_gate, near_up, near_low, near_high),
            (far_gate, far_up, far_low, far_high),
            near_far,
        ),
    )
    return return_rows(routed.reshape(sp, rows_dev, width), shared_out, stream, sp, tp, 4)


def solution(mesh):
    in_specs = (
        P("sp", "tp"),
        P("sp", "tp"),
        P("sp", "tp"),
        P("tp"),
        P(),
        P(),
        P(("sp", "tp"), None),
        P(),
        P("sp", None),
        P(("sp", "tp"), None),
        P("sp", None, "tp"),
        P("sp", None, "tp"),
        P("sp", "tp", None),
        P(None, "tp"),
        P(None, "tp"),
        P("tp", None),
    )
    out_specs = P(("sp", "tp"), None)
    sp, tp = mesh.shape["sp"], mesh.shape["tp"]

    def chosen(*args):
        route_count = args[8].shape[1]
        experts = sp * args[10].shape[0]
        rows_dev = args[6].shape[0]
        whole_blocks = 2 * rows_dev * route_count >= experts * rows_dev
        dense = whole_blocks and args[10].shape[0] == 1 and sp == 8 and tp == 4
        if not dense:
            return body(*args)
        return dense_body(*args)

    return jax.shard_map(
        chosen, mesh=mesh, in_specs=in_specs, out_specs=out_specs, check_vma=False
    )
```
